32 devices in a mesh: rep: 4 (over z), fs: 2 (over y), tp: 4 (over x, core).
Axes of the slice: x: 2, y: 2, z: 4, core: 2. Of those that a mesh axis runs over, the one named last changes fastest.
Arguments:
- inputs: bfloat16 [512, 4096], P('rep'), may hold values from -6 to 6
- cotangent: bfloat16 [512, 4096], P('rep'), may hold values from -6 to 6
- w_gate: bfloat16 [4096, 11264], P(None, ('fs', 'tp')), may hold values from -0.09375 to 0.09375
- w_upward: bfloat16 [4096, 11264], P(None, ('fs', 'tp')), may hold values from -0.09375 to 0.09375
- w_down: bfloat16 [11264, 4096], P(('fs', 'tp')), may hold values from -0.0546875 to 0.0546875
Outputs:
- grad_input: bfloat16 [512, 4096], P('rep')
- grad_gate: float32 [4096, 11264], P('rep', ('fs', 'tp'))
- grad_upward: float32 [4096, 11264], P('rep', ('fs', 'tp'))
- grad_down: float32 [11264, 4096], P(('fs', 'tp'), 'rep')
The draws below stay inside these ranges and needn't reach their ends.
All inputs are finite; a program needn't handle non-finite values.
Results may differ from the reference program's by a relative error of at most 0.0049.
Values may be sent and summed in bfloat16 or wider, within the bound.
A program may use at most 128 MiB of HBM per device.

```python
import jax
import jax.numpy as jnp

D = 4096
FF = 11264
TOKENS = 512


def spiked(result, rng, source, target, parts, factor):
    owner, partner = [(jnp.arange(result.shape[position]) // (result.shape[position] // parts)).reshape([-1 if axis == position else 1 for axis in range(result.ndim)]) for position in (source, target)]
    chosen = jax.random.permutation(rng, parts)[partner]
    strong = (owner == chosen) | (owner == (partner + parts // 2) % parts)
    return jnp.where(strong, factor * result, result)


def shard_levels(stream_key, extent, split, smallest, largest):
    loudness, own = 1.0, jax.random.fold_in(stream_key, 6)
    for position, shards_of in split:
        draws = jnp.exp(jax.random.uniform(jax.random.fold_in(own, position), (shards_of,), jnp.float32, smallest / len(split), largest / len(split)))
        loudness = loudness * jnp.repeat(draws, extent[position] // shards_of).reshape([-1 if axis == position else 1 for axis in range(len(extent))])
    return loudness


def centred(rng, shape, spread, reach, pieces=(), dtype=jnp.bfloat16):
    values = jax.random.normal(rng, shape, jnp.float32) * spread
    if len(pieces) > 0:
        values = shard_levels(rng, shape, pieces, -0.22, 0.18) * values
    return jnp.clip(values, min=-reach, max=reach).astype(dtype)


def bell_draw_with(own_key, dims, scale, limit, split, heavy, dtype=jnp.bfloat16):
    drawn = scale * jax.random.normal(own_key, dims, jnp.float32)
    if split:
        drawn = drawn * shard_levels(own_key, dims, split, -0.22, 0.18)
    return jnp.clip(spiked(drawn, jax.random.fold_in(own_key, 3), *heavy), -limit, limit).astype(dtype)


def setup_inputs(seed: int = 0) -> dict:
    keys = jax.random.split(jax.random.key(seed), 6)
    inputs = centred(keys[0], (TOKENS, D), 1.0, 6.0, ((0, 4),))
    cotangent = bell_draw_with(keys[1], (TOKENS, D), 1.0, 6.0, ((0, 4),), (0, 1, 4, 2.0))
    w_gate = centred(keys[2], (D, FF), D ** -0.5, 0.09375, ((1, 8),))
    w_upward = centred(keys[3], (D, FF), D ** -0.5, 0.09375, ((1, 8),))
    w_down = centred(keys[4], (FF, D), FF ** -0.5, 0.0546875, ((0, 8),))
    return {"inputs": inputs, "cotangent": cotangent, "w_gate": w_gate, "w_upward": w_upward, "w_down": w_down}


def reference(inputs, cotangent, w_gate, w_upward, w_down):
    gate_pre = jnp.dot(inputs, w_gate, preferred_element_type=jnp.float32)
    up_pre = jnp.dot(inputs, w_upward, preferred_element_type=jnp.float32)
    sigmoid_gate = jax.nn.sigmoid(gate_pre)
    activated = gate_pre * sigmoid_gate
    hidden = (activated * up_pre).astype(jnp.bfloat16)
    hidden_grad = jnp.dot(cotangent, w_down.T, preferred_element_type=jnp.float32)
    gate_delta = (hidden_grad * up_pre * sigmoid_gate * (1.0 + gate_pre * (1.0 - sigmoid_gate))).astype(jnp.bfloat16)
    up_delta = (hidden_grad * activated).astype(jnp.bfloat16)
    grad_input = (jnp.dot(gate_delta, w_gate.T, preferred_element_type=jnp.float32)
                  + jnp.dot(up_delta, w_upward.T, preferred_element_type=jnp.float32)).astype(jnp.bfloat16)
    grad_gate = jnp.dot(inputs.T, gate_delta, preferred_element_type=jnp.float32)
    grad_upward = jnp.dot(inputs.T, up_delta, preferred_element_type=jnp.float32)
    grad_down = jnp.dot(hidden.T, cotangent, preferred_element_type=jnp.float32)
    return (grad_input, grad_gate, grad_upward, grad_down)
```

```python
import jax
import jax.numpy as jnp
from jax import lax
from jax.sharding import PartitionSpec as P

PLANE = ("fs", "tp")


def contract_rows(left, right):
    return lax.dot_general(
        left, right, (((0,), (0,)), ((), ())), preferred_element_type=jnp.float32
    )


def contract_cols(left, right):
    return lax.dot_general(
        left, right, (((1,), (1,)), ((), ())), preferred_element_type=jnp.float32
    )


def forward(inputs, cotangent, w_gate, w_upward, w_down):
    gate_pre = jnp.dot(inputs, w_gate, preferred_element_type=jnp.float32)
    up_pre = jnp.dot(inputs, w_upward, preferred_element_type=jnp.float32)
    sigmoid_gate = jax.nn.sigmoid(gate_pre)
    activated = gate_pre * sigmoid_gate
    hidden = (activated * up_pre).astype(jnp.bfloat16)
    hidden_grad = contract_cols(cotangent, w_down)
    gate_delta = (
        hidden_grad * up_pre * sigmoid_gate * (1.0 + gate_pre * (1.0 - sigmoid_gate))
    ).astype(jnp.bfloat16)
    up_delta = (hidden_grad * activated).astype(jnp.bfloat16)
    return gate_delta, up_delta, hidden


def local(planes, inputs, cotangent, w_gate, w_upward, w_down):
    rows, width = inputs.shape
    share = rows // planes
    me = lax.axis_index(PLANE)
    mine = [lax.dynamic_slice_in_dim(a, me * share, share, 0) for a in (inputs, cotangent)]
    everyone = ("rep",) + PLANE
    all_inputs, all_cotangent = [lax.all_gather(a, everyone, axis=0, tiled=True) for a in mine]

    gate_delta, up_delta, _ = forward(inputs, cotangent, w_gate, w_upward, w_down)
    terms = contract_cols(gate_delta, w_gate) + contract_cols(up_delta, w_upward)
    terms = terms.astype(jnp.bfloat16)
    terms = lax.all_to_all(terms.reshape(planes, share, width), PLANE, 0, 0)
    total = jnp.sum(terms.astype(jnp.float32), axis=0).astype(jnp.bfloat16)
    grad_input = lax.all_gather(total, PLANE, axis=0, tiled=True)

    gate_delta, up_delta, hidden = forward(all_inputs, all_cotangent, w_gate, w_upward, w_down)
    reps = all_inputs.shape[0] // rows
    cols = width // reps
    at = lax.axis_index("rep") * cols
    input_cols = lax.dynamic_slice_in_dim(all_inputs, at, cols, 1)
    cotangent_cols = lax.dynamic_slice_in_dim(all_cotangent, at, cols, 1)
    grad_gate = contract_rows(input_cols, gate_delta)
    grad_upward = contract_rows(input_cols, up_delta)
    grad_down = contract_rows(hidden, cotangent_cols)
    return (grad_input, grad_gate, grad_upward, grad_down)


def solution(mesh):
    planes = mesh.shape["fs"] * mesh.shape["tp"]
    in_specs = (
        P("rep", None),
        P("rep", None),
        P(None, PLANE),
        P(None, PLANE),
        P(PLANE, None),
    )
    out_specs = (
        P("rep", None),
        P("rep", PLANE),
        P("rep", PLANE),
        P(PLANE, "rep"),
    )

    def body(*args):
        return local(planes, *args)

    return jax.shard_map(body, mesh=mesh, in_specs=in_specs, out_specs=out_specs, check_vma=False)
```

```python
import functools

import jax
import jax.numpy as jnp
from jax import lax
from jax.experimental import pallas as pl
from jax.experimental.pallas import tpu as pltpu
from jax.sharding import PartitionSpec as P

PLANE = ("fs", "tp")
MESH = pl.DeviceIdType.MESH


def contract_rows(left, right):
    return lax.dot_general(
        left, right, (((0,), (0,)), ((), ())), preferred_element_type=jnp.float32
    )


def contract_cols(left, right):
    return lax.dot_general(
        left, right, (((1,), (1,)), ((), ())), preferred_element_type=jnp.float32
    )


def greet(neighbours):
    barrier = pltpu.get_barrier_semaphore()
    for device in neighbours:
        pl.semaphore_signal(barrier, inc=1, device_id=device, device_id_type=MESH)
    pl.semaphore_wait(barrier, len(neighbours))


def gather_kernel(reps, x_ref, c_ref, all_x, all_c, send, recv, own_sem):
    z, y, t = lax.axis_index("rep"), lax.axis_index("fs"), lax.axis_index("tp")
    x, core = t // 2, t % 2
    half = (x + y) % 2
    mine = 2 * half + core
    across = 2 * (1 - half) + core
    up, down = (z + 1) % reps, (z + reps - 1) % reps
    to_up, to_down = (up, y, t), (down, y, t)
    x_near = (z, y, 2 * (x + 1 - 2 * (x % 2)) + core)
    y_near = (z, y + 1 - 2 * (y % 2), t)
    other = (z, y, 2 * x + 1 - core)
    greet((to_up, to_down, x_near, y_near, other))

    started = []

    def put(kind, step, src, dst, device):
        copy = pltpu.make_async_remote_copy(
            src_ref=src, dst_ref=dst, send_sem=send.at[kind, step],
            recv_sem=recv.at[kind, step], device_id=device, device_id_type=MESH,
        )
        copy.start()
        started.append(copy)
        return copy

    ring = [
        put(0, 0, x_ref.at[mine], all_x.at[z, mine], to_up),
        put(1, 0, c_ref.at[mine], all_c.at[z, mine], to_down),
    ]
    keep = [
        pltpu.make_async_copy(x_ref, all_x.at[z], own_sem.at[0]),
        pltpu.make_async_copy(c_ref, all_c.at[z], own_sem.at[1]),
    ]
    for copy in keep:
        copy.start()

    last = []

    def relay(sides, step, bx, bc):
        sides[0].wait_recv()
        last.append(put(6, step, all_x.at[bx, across], all_x.at[bx, across], other))
        sides[1].wait_recv()
        last.append(put(7, step, all_c.at[bc, across], all_c.at[bc, across], other))

    before = None
    for step in range(reps - 1):
        bx, bc = (z + reps - 1 - step) % reps, (z + 1 + step) % reps
        got_x, got_c = all_x.at[bx, mine], all_c.at[bc, mine]
        following = []
        ring[0].wait_recv()
        if step < reps - 2:
            following.append(put(0, step + 1, got_x, got_x, to_up))
        side_x = put(2, step, got_x, got_x, x_near)
        last.append(put(4, step, got_x, got_x, other))
        ring[1].wait_recv()
        if step < reps - 2:
            following.append(put(1, step + 1, got_c, got_c, to_down))
        side_c = put(3, step, got_c, got_c, y_near)
        last.append(put(5, step, got_c, got_c, other))
        if before is not None:
            relay(*before)
        before = ((side_x, side_c), step, bx, bc)
        ring = following
    relay(*before)
    for copy in last:
        copy.wait_recv()
    for copy in started:
        copy.wait_send()
    for copy in keep:
        copy.wait()


def gather(reps, inputs, cotangent):
    rows, width = inputs.shape
    quarter = (4, rows // 4, width)
    whole = jax.ShapeDtypeStruct((reps,) + quarter, inputs.dtype)
    vmem = pl.BlockSpec(memory_space=pltpu.VMEM)
    pair = pl.pallas_call(
        functools.partial(gather_kernel, reps),
        out_shape=(whole, whole),
        in_specs=[vmem, vmem],
        out_specs=(vmem, vmem),
        scratch_shapes=[
            pltpu.SemaphoreType.DMA((8, reps - 1)),
            pltpu.SemaphoreType.DMA((8, reps - 1)),
            pltpu.SemaphoreType.DMA((2,)),
        ],
        compiler_params=pltpu.CompilerParams(
            collective_id=0, has_side_effects=True, vmem_limit_bytes=60 * 2**20
        ),
        name="token_gather",
    )(inputs.reshape(quarter), cotangent.reshape(quarter))
    return [a.reshape(reps * rows, width) for a in pair]


def reduce_kernel(chips, across, terms, out, got, sums, landed, send, recv):
    z, y, t = lax.axis_index("rep"), lax.axis_index("fs"), lax.axis_index("tp")
    core = t % 2
    chip = y * across + t // 2
    other = (z, y, t + 1 - 2 * core)

    def peer(ahead):
        there = (chip + ahead) % chips
        return there, (z, there // across, 2 * (there % across) + core)

    greet([other] + [peer(ahead)[1] for ahead in range(1, chips)])

    def put(kind, slot, src, dst, device):
        copy = pltpu.make_async_remote_copy(
            src_ref=src, dst_ref=dst, send_sem=send.at[kind, slot],
            recv_sem=recv.at[kind, slot], device_id=device, device_id_type=MESH,
        )
        copy.start()
        return copy

    swaps = [put(0, j, terms.at[j, 1 - core], got.at[j], other) for j in range(chips)]
    for j in range(chips):
        swaps[j].wait_recv()
        pair = terms[j, core].astype(jnp.float32) + got[j].astype(jnp.float32)
        sums[j] = pair.astype(sums.dtype)
    spread = []
    for ahead in range(1, chips):
        there, device = peer(ahead)
        spread.append(put(1, ahead, sums.at[there], landed.at[ahead], device))
    total = terms[chip, core].astype(jnp.float32) + got[chip].astype(jnp.float32)
    for ahead in range(1, chips):
        spread[ahead - 1].wait_recv()
        total = total + landed[ahead].astype(jnp.float32)
    out[chip, core] = total.astype(out.dtype)
    done = out.at[chip, core]
    share = [put(2, ahead, done, done, peer(ahead)[1]) for ahead in range(1, chips)]
    relays = [put(3, 0, done, done, other)]
    for ahead in range(1, chips):
        share[ahead - 1].wait_recv()
        source = out.at[(chip + chips - ahead) % chips, core]
        relays.append(put(3, ahead, source, source, other))
    for copy in relays:
        copy.wait_recv()
    for copy in swaps + spread + share + relays:
        copy.wait_send()


def plane_sum(chips, across, terms):
    rows, width = terms.shape
    piece = (rows // (2 * chips), width)
    vmem = pl.BlockSpec(memory_space=pltpu.VMEM)
    total = pl.pallas_call(
        functools.partial(reduce_kernel, chips, across),
        out_shape=jax.ShapeDtypeStruct((chips, 2) + piece, terms.dtype),
        in_specs=[vmem],
        out_specs=vmem,
        scratch_shapes=[
            pltpu.VMEM((chips,) + piece, terms.dtype),
            pltpu.VMEM((chips,) + piece, terms.dtype),
            pltpu.VMEM((chips,) + piece, terms.dtype),
            pltpu.SemaphoreType.DMA((4, chips)),
            pltpu.SemaphoreType.DMA((4, chips)),
        ],
        compiler_params=pltpu.CompilerParams(
            collective_id=1, has_side_effects=True, vmem_limit_bytes=48 * 2**20
        ),
        name="plane_sum",
    )(terms.reshape((chips, 2) + piece))
    return total.reshape(rows, width)


def local(reps, chips, across, inputs, cotangent, w_gate, w_upward, w_down):
    rows, width = inputs.shape
    all_inputs, all_cotangent = gather(reps, inputs, cotangent)

    gate_pre = jnp.dot(all_inputs, w_gate, preferred_element_type=jnp.float32)
    up_pre = jnp.dot(all_inputs, w_upward, preferred_element_type=jnp.float32)
    sigmoid_gate = jax.nn.sigmoid(gate_pre)
    activated = gate_pre * sigmoid_gate
    hidden = (activated * up_pre).astype(jnp.bfloat16)
    hidden_grad = contract_cols(all_cotangent, w_down)
    gate_delta = (
        hidden_grad * up_pre * sigmoid_gate * (1.0 + gate_pre * (1.0 - sigmoid_gate))
    ).astype(jnp.bfloat16)
    up_delta = (hidden_grad * activated).astype(jnp.bfloat16)

    z = lax.axis_index("rep")
    own_gate = lax.dynamic_slice_in_dim(gate_delta, z * rows, rows, 0)
    own_up = lax.dynamic_slice_in_dim(up_delta, z * rows, rows, 0)
    terms = contract_cols(own_gate, w_gate) + contract_cols(own_up, w_upward)
    grad_input = plane_sum(chips, across, terms.astype(jnp.bfloat16))

    cols = width // reps
    input_cols = lax.dynamic_slice_in_dim(all_inputs, z * cols, cols, 1)
    cotangent_cols = lax.dynamic_slice_in_dim(all_cotangent, z * cols, cols, 1)
    grad_gate = contract_rows(input_cols, gate_delta)
    grad_upward = contract_rows(input_cols, up_delta)
    grad_down = contract_rows(hidden, cotangent_cols)
    return (grad_input, grad_gate, grad_upward, grad_down)


def solution(mesh):
    across = mesh.shape["tp"] // 2
    chips = mesh.shape["fs"] * across
    in_specs = (
        P("rep", None),
        P("rep", None),
        P(None, PLANE),
        P(None, PLANE),
        P(PLANE, None),
    )
    out_specs = (
        P("rep", None),
        P("rep", PLANE),
        P("rep", PLANE),
        P(PLANE, "rep"),
    )
    body = functools.partial(local, mesh.shape["rep"], chips, across)
    return jax.shard_map(body, mesh=mesh, in_specs=in_specs, out_specs=out_specs, check_vma=False)
```
